256 devices in a mesh: fs: 32 (over z, y), tp: 8 (over x, core).
Axes of the slice: x: 4, y: 4, z: 8, core: 2. Of those that a mesh axis runs over, the one named last changes fastest.
Arguments:
- cotangent: bfloat16 [32768, 4096], P(('fs', 'tp')), may hold values from -24 to 24
- gate_pre: bfloat16 [32768, 6144], P('fs', 'tp'), may hold values from -8 to 8
- up_pre: bfloat16 [32768, 6144], P('fs', 'tp'), may hold values from -6 to 6
- down_weight: bfloat16 [4096, 6144], P('fs', 'tp'), may hold values from -0.078125 to 0.078125
Outputs:
- gate_grad: bfloat16 [32768, 6144], P('fs', 'tp')
- up_grad: bfloat16 [32768, 6144], P('fs', 'tp')
- down_grad: float32 [4096, 6144], P('fs', 'tp')
The draws below stay inside these ranges and needn't reach their ends.
All inputs are finite; a program needn't handle non-finite values.
Results may differ from the reference program's by a relative error of at most 0.0027.
Values may be sent and summed in bfloat16 or wider, within the bound.
No kernel may reach another device: no remote copies, remote signals or barrier semaphores. Data moves between devices by JAX's collectives and lax.ppermute only.
A program may use at most 128 MiB of HBM per device.

```python
import math
import jax
import jax.numpy as jnp
from jax import lax

D = 4096
FF = 6144
TOKENS = 32768


def raised(array, rng, source, target, parts, factor):
    def block_of(dim):
        return (jnp.arange(array.shape[dim]) // (array.shape[dim] // parts)).reshape((-1,) + (1,) * (array.ndim - 1 - dim))

    first = jax.random.permutation(rng, parts)[block_of(target)]
    second = (block_of(target) + parts // 2) % parts
    return jnp.where((block_of(source) == first) | (block_of(source) == second), factor * array, array)


def block_scale(rng, dims, pieces, least, largest):
    gain = 1.0
    for axis_at, blocks in pieces:
        steps = jax.random.uniform(jax.random.fold_in(jax.random.fold_in(rng, 6), axis_at), (blocks,), jnp.float32, least / len(pieces), largest / len(pieces))
        gain = gain * jnp.repeat(jnp.exp(steps), dims[axis_at] // blocks).reshape((-1,) + (1,) * (len(dims) - 1 - axis_at))
    return gain


def noise(rng, shape, scale, most, cuts=(), kind=jnp.bfloat16):
    entries = jax.random.normal(rng, shape, jnp.float32) * scale
    if len(cuts) > 0:
        entries = block_scale(rng, shape, cuts, -0.22, 0.18) * entries
    return jnp.clip(entries, min=-most, max=most).astype(kind)


def gaussian_with(stream_key, dims, scale, limit, cuts, heavy, held_as=jnp.bfloat16):
    drawn = scale * jax.random.normal(stream_key, dims, jnp.float32)
    if cuts:
        drawn = drawn * block_scale(stream_key, dims, cuts, -0.22, 0.18)
    return jnp.clip(raised(drawn, jax.random.fold_in(stream_key, 3), *heavy), -limit, limit).astype(held_as)


def setup_inputs(seed: int = 0) -> dict:
    splits = jax.random.split(jax.random.key(seed), 5)
    cotangent = gaussian_with(splits[0], (TOKENS, D), 1.0, 24.0, ((0, 256),), (0, 1, 256, 6.0))
    gate_pre = noise(splits[1], (TOKENS, FF), 1.5, 8.0, ((0, 32), (1, 8)))
    up_pre = noise(splits[2], (TOKENS, FF), 1.0, 6.0, ((0, 32), (1, 8)))
    down_weight = noise(splits[3], (D, FF), FF ** -0.5, 0.078125, ((0, 32), (1, 8)))
    return dict(cotangent=cotangent, gate_pre=gate_pre, up_pre=up_pre, down_weight=down_weight)


def reference(cotangent, gate_pre, up_pre, down_weight):
    gate_values = gate_pre.astype(jnp.float32)
    up_values = up_pre.astype(jnp.float32)
    sigmoid_gate = jax.nn.sigmoid(gate_values)
    silu_gate = gate_values * sigmoid_gate
    hidden = (silu_gate * up_values).astype(jnp.bfloat16)
    hidden_grad = 0.5 * jnp.dot(cotangent, down_weight, preferred_element_type=jnp.float32)
    up_grad = (hidden_grad * silu_gate).astype(jnp.bfloat16)
    gate_grad = (hidden_grad * up_values * sigmoid_gate * (1.0 + gate_values * (1.0 - sigmoid_gate))).astype(jnp.bfloat16)
    product = lax.dot_general(cotangent, hidden, (((0,), (0,)), ((), ())), preferred_element_type=jnp.float32)
    down_grad = product * (0.5 / math.sqrt(TOKENS))
    return (gate_grad, up_grad, down_grad)
```

```python
import math

import jax
import jax.numpy as jnp
from jax import lax
from jax.experimental import pallas as pl
from jax.experimental.pallas import tpu as pltpu
from jax.sharding import Mesh
from jax.sharding import PartitionSpec as P


BF16 = jnp.bfloat16
F32 = jnp.float32
NZ, NY, NX, NC = 8, 4, 4, 2
PARAMS = pltpu.CompilerParams(vmem_limit_bytes=56 * 1024 * 1024)


def shift(value, axis, step):
    size = lax.axis_size(axis)
    return lax.ppermute(value, axis, [(i, (i + step) % size) for i in range(size)])


def swap(value):
    return lax.ppermute(value, "c", [(0, 1), (1, 0)])


def arrange_kernel(order, source, top, bottom):
    for j in range(NZ * NY):
        start = pl.multiple_of(order[j] * 128, 128)
        at = slice(j * 128, (j + 1) * 128)
        top[:, at] = source[:64, pl.ds(start, 128)]
        bottom[:, at] = source[64:, pl.ds(start, 128)]


def arrange(cotangent, order):
    half = (cotangent.shape[0] // 2, cotangent.shape[1])
    return pl.pallas_call(
        arrange_kernel,
        out_shape=[jax.ShapeDtypeStruct(half, cotangent.dtype)] * 2,
        grid_spec=pltpu.PrefetchScalarGridSpec(
            num_scalar_prefetch=1,
            grid=(1,),
            in_specs=[pl.BlockSpec(cotangent.shape, lambda i, o: (0, 0))],
            out_specs=[pl.BlockSpec(half, lambda i, o: (0, 0))] * 2,
        ),
        compiler_params=PARAMS,
        name="arrange",
    )(order, cotangent)


def hidden_kernel(gate, up, out):
    gate_values = gate[...].astype(F32)
    hidden = gate_values * jax.nn.sigmoid(gate_values) * up[...].astype(F32)
    out[...] = hidden.T.astype(BF16)


def hidden_transposed(gate_pre, up_pre):
    tokens, width = gate_pre.shape
    return pl.pallas_call(
        hidden_kernel,
        out_shape=jax.ShapeDtypeStruct((width, tokens), BF16),
        grid=(tokens // 256,),
        in_specs=[pl.BlockSpec((256, width), lambda i: (i, 0))] * 2,
        out_specs=pl.BlockSpec((width, 256), lambda i: (0, i)),
        compiler_params=PARAMS,
        name="hidden",
    )(gate_pre, up_pre)


def write_sums(product, right, left, mine, ahead, behind):
    low = pl.program_id(0) < NZ // 4
    for q in range(2):
        part = [product[:, q * 512 + j * 128 : q * 512 + (j + 1) * 128] for j in range(NY)]
        at = slice(q * 128, (q + 1) * 128)
        mine[:, at] = part[0]

        @pl.when(low)
        def _():
            right[:, at] = part[2].astype(BF16)
            left[:, at] = part[3].astype(BF16)
            ahead[:, at] = part[1]

        @pl.when(jnp.logical_not(low))
        def _():
            right[:, at] = part[1].astype(BF16)
            left[:, at] = part[2].astype(BF16)
            behind[:, at] = part[3]


def first_kernel(order, hidden, *refs):
    blocks, packed, outs = refs[:16], refs[16], refs[17:]
    for b, block in enumerate(blocks):
        at = pl.ds(pl.multiple_of(order[b // 2] * 128 + (b % 2) * 64, 64), 64)
        packed[at, :] = block[...]
    write_sums(jnp.dot(hidden[...], packed[...], preferred_element_type=F32), *outs)


def second_kernel(hidden, packed, *outs):
    write_sums(jnp.dot(hidden[...], packed[...], preferred_element_type=F32), *outs)


def sum_specs(half):
    wide, narrow = (half, NZ * 128), (half, NZ * 64)
    outs = [(wide, BF16), (wide, BF16), (wide, F32), (narrow, F32), (narrow, F32)]
    specs = [pl.BlockSpec((half, 256), lambda i, *_: (0, i))] * 3
    specs.append(pl.BlockSpec((half, 256), lambda i, *_: (0, jnp.minimum(i, 1))))
    specs.append(pl.BlockSpec((half, 256), lambda i, *_: (0, jnp.maximum(i - 2, 0))))
    return [jax.ShapeDtypeStruct(*out) for out in outs], specs


def first_sums(hidden, blocks, order):
    half, tokens = hidden.shape[0] // 2, hidden.shape[1]
    shapes, specs = sum_specs(half)
    width = blocks[0].shape[1]
    return pl.pallas_call(
        first_kernel,
        out_shape=[jax.ShapeDtypeStruct((tokens, width), BF16)] + shapes,
        grid_spec=pltpu.PrefetchScalarGridSpec(
            num_scalar_prefetch=1,
            grid=(NZ // 2,),
            in_specs=[pl.BlockSpec((half, tokens), lambda i, o: (0, 0))]
            + [pl.BlockSpec((64, width * 2 // NZ), lambda i, o: (0, i))] * len(blocks),
            out_specs=[pl.BlockSpec((tokens, width * 2 // NZ), lambda i, o: (0, i))] + specs,
        ),
        compiler_params=PARAMS,
        cost_estimate=pl.CostEstimate(flops=2 * half * tokens * width, bytes_accessed=24 << 20, transcendentals=0),
        name="first_sums",
    )(order, hidden, *blocks)


def second_sums(hidden, packed):
    half, tokens = hidden.shape[0] // 2, hidden.shape[1]
    shapes, specs = sum_specs(half)
    width = packed.shape[1]
    return pl.pallas_call(
        second_kernel,
        out_shape=shapes,
        grid=(NZ // 2,),
        in_specs=[
            pl.BlockSpec((half, tokens), lambda i: (1, 0)),
            pl.BlockSpec((tokens, width * 2 // NZ), lambda i: (0, i)),
        ],
        out_specs=specs,
        compiler_params=PARAMS,
        cost_estimate=pl.CostEstimate(flops=2 * half * tokens * width, bytes_accessed=16 << 20, transcendentals=0),
        name="second_sums",
    )(hidden, packed)


def input_grad_kernel(where, gate, up, columns, *refs):
    weights, (gate_out, up_out) = refs[:NZ], refs[NZ:]
    total = None
    for k, w in enumerate(weights):
        at = pl.ds(pl.multiple_of(where[k] * 512, 512), 512)
        term = jnp.dot(columns[:, at], w[...], preferred_element_type=F32)
        total = term if total is None else total + term
    grad = total * 0.5
    gate_values = gate[...].astype(F32)
    up_values = up[...].astype(F32)
    sig = jax.nn.sigmoid(gate_values)
    up_out[...] = (grad * (gate_values * sig)).astype(BF16)
    gate_out[...] = (grad * up_values * sig * (1.0 + gate_values * (1.0 - sig))).astype(BF16)


def input_grads(gate_pre, up_pre, packed, weights, where):
    tokens, width = gate_pre.shape
    rows = 256
    tile = pl.BlockSpec((rows, width), lambda i, o: (i, 0))
    return pl.pallas_call(
        input_grad_kernel,
        out_shape=[jax.ShapeDtypeStruct((tokens, width), BF16)] * 2,
        grid_spec=pltpu.PrefetchScalarGridSpec(
            num_scalar_prefetch=1,
            grid=(tokens // rows,),
            in_specs=[tile, tile, pl.BlockSpec((rows, packed.shape[1]), lambda i, o: (i, 0))]
            + [pl.BlockSpec(w.shape, lambda i, o: (0, 0)) for w in weights],
            out_specs=[tile, tile],
        ),
        compiler_params=PARAMS,
        cost_estimate=pl.CostEstimate(
            flops=2 * tokens * width * packed.shape[1], bytes_accessed=24 << 20, transcendentals=0
        ),
        name="input_grads",
    )(where, gate_pre, up_pre, packed, *weights)


def join_kernel(*refs):
    for k, ref in enumerate(refs[:-1]):
        refs[-1][k * 128 : (k + 1) * 128, :] = ref[...]


def join(parts):
    rows, width = parts[0].shape
    return pl.pallas_call(
        join_kernel,
        out_shape=jax.ShapeDtypeStruct((rows * len(parts), width), parts[0].dtype),
        compiler_params=PARAMS,
        name="join",
    )(*parts)


def gather_tokens(top, bottom):
    behind_top = shift(top, "x", 1)
    ahead_bottom = shift(bottom, "x", -1)
    behind_bottom = shift(bottom, "x", 1)
    ahead_top = shift(top, "x", -1)
    far_top = shift(behind_top, "x", 1)
    far_bottom = shift(ahead_bottom, "x", -1)
    blocks = []
    for half in ((top, bottom), (behind_top, behind_bottom), (ahead_top, ahead_bottom), (far_top, far_bottom)):
        blocks.extend(half)
        blocks.extend(swap(h) for h in half)
    return blocks


def gather_weights(weight):
    behind = shift(weight, "y", 1)
    ahead = shift(weight, "y", -1)
    far = shift(weight, "y", 2)
    here = join([weight, ahead, far, behind])
    parts = {0: here}
    up, down = here, here
    for hop in range(1, 5):
        up = shift(up, "z", 1)
        parts[(-hop) % NZ] = up
        if hop < 4:
            down = shift(down, "z", -1)
            parts[hop] = down
    return [parts[k] for k in range(NZ)]


def sum_over_fs(right, left, mine, ahead, behind):
    half = mine.shape[1] // 2
    right = shift(right, "y", 1)
    left = shift(left, "y", -1)
    up = shift((ahead + right[:, :half].astype(F32)).astype(BF16), "y", 1)
    down = shift((behind + left[:, half:].astype(F32)).astype(BF16), "y", -1)
    pieces = pl.pallas_call(
        pieces_kernel,
        out_shape=jax.ShapeDtypeStruct((NZ, mine.shape[0], 128), BF16),
        compiler_params=PARAMS,
        name="pieces",
    )(mine, right, left, up, down)
    pieces = lax.all_to_all(pieces, "z", 0, 0)
    return jnp.sum(pieces.astype(F32), axis=0)


def pieces_kernel(mine, right, left, up, down, out):
    half = mine.shape[1] // 2
    for k in range(NZ):
        at = slice(k * 128, (k + 1) * 128)
        there = slice(k * 128 % half, k * 128 % half + 128)
        one, two = (up[:, there], left[:, at]) if k < 4 else (right[:, at], down[:, there])
        out[k] = (mine[:, at] + one.astype(F32) + two.astype(F32)).astype(BF16)


def step(cotangent, gate_pre, up_pre, down_weight):
    z, y, x, c = (lax.axis_index(a) for a in ("z", "y", "x", "c"))
    token_total = gate_pre.shape[0] * NZ * NY
    grad_scale = 0.5 / math.sqrt(token_total)
    steps = jnp.arange(NZ * NY, dtype=jnp.int32)
    features = (steps // NY) * NY + (y + steps % NY) % NY
    distance = jnp.array([0, 0, 3, 3, 1, 1, 2, 2], jnp.int32)
    other = jnp.array([0, 1, 0, 1, 0, 1, 0, 1], jnp.int32)
    tokens = ((x + distance) % NX) * NC + (c + other) % NC
    where = (z + jnp.arange(NZ, dtype=jnp.int32)) % NZ

    blocks = gather_tokens(*arrange(cotangent, features.astype(jnp.int32)))
    weights = gather_weights(down_weight)
    hidden = hidden_transposed(gate_pre, up_pre)
    packed, *sums = first_sums(hidden, blocks, tokens.astype(jnp.int32))
    first = sum_over_fs(*sums)
    sums = second_sums(hidden, packed)
    second = sum_over_fs(*sums)
    gate_grad, up_grad = input_grads(gate_pre, up_pre, packed, weights, where.astype(jnp.int32))
    down_grad = jnp.concatenate([first, second], axis=0).T * grad_scale
    return gate_grad, up_grad, down_grad


def solution(mesh):
    torus = Mesh(mesh.devices.reshape(NZ, NY, NX, NC), ("z", "y", "x", "c"))
    fs, tp = ("z", "y"), ("x", "c")
    return jax.shard_map(
        step,
        mesh=torus,
        in_specs=(P(fs + tp, None), P(fs, tp), P(fs, tp), P(fs, tp)),
        out_specs=(P(fs, tp), P(fs, tp), P(fs, tp)),
        check_vma=False,
    )
```

```python
import math

import jax
import jax.numpy as jnp
from jax import lax
from jax.experimental import pallas as pl
from jax.experimental.pallas import tpu as pltpu
from jax.sharding import Mesh
from jax.sharding import PartitionSpec as P


BF16 = jnp.bfloat16
F32 = jnp.float32
NZ, NY, NX, NC = 8, 4, 4, 2
PARAMS = pltpu.CompilerParams(vmem_limit_bytes=56 * 1024 * 1024)


def shift(value, axis, step):
    size = lax.axis_size(axis)
    return lax.ppermute(value, axis, [(i, (i + step) % size) for i in range(size)])


def swap(value):
    return lax.ppermute(value, "c", [(0, 1), (1, 0)])


def hidden_kernel(gate, up, out):
    gate_values = gate[...].astype(F32)
    hidden = gate_values * jax.nn.sigmoid(gate_values) * up[...].astype(F32)
    out[...] = hidden.T.astype(BF16)


def hidden_transposed(gate_pre, up_pre, pairs):
    tokens, width = gate_pre.shape
    return pl.pallas_call(
        lambda order, gate, up, out: hidden_kernel(gate, up, out),
        out_shape=jax.ShapeDtypeStruct((width, tokens), BF16),
        grid_spec=pltpu.PrefetchScalarGridSpec(
            num_scalar_prefetch=1,
            grid=(tokens // 256,),
            in_specs=[pl.BlockSpec((256, width), lambda i, o: (o[i], 0))] * 2,
            out_specs=pl.BlockSpec((width, 256), lambda i, o: (0, i)),
        ),
        compiler_params=PARAMS,
        name="hidden",
    )(pairs, gate_pre, up_pre)


def pack(place, blocks, packed):
    for b, block in enumerate(blocks):
        pair, rest = divmod(b, 4)
        core, half = divmod(rest, 2)
        row = pair * 256 + (place[0] + core) % 2 * 128 + half * 64
        at = pl.ds(pl.multiple_of(row, 64), 64)
        for j in range(NY):
            lane = (place[1] + j) % NY * 128
            for q in range(2):
                here = pl.ds(pl.multiple_of(q * 512 + lane, 128), 128)
                packed[at, q * 512 + j * 128 : q * 512 + (j + 1) * 128] = block[:, here]


def write_sums(product, right, left, mine, ahead, behind):
    low = pl.program_id(0) < NZ // 4
    for q in range(2):
        part = [product[:, q * 512 + j * 128 : q * 512 + (j + 1) * 128] for j in range(NY)]
        at = slice(q * 128, (q + 1) * 128)
        mine[:, at] = part[0]

        @pl.when(low)
        def _():
            right[:, at] = part[2].astype(BF16)
            left[:, at] = part[3].astype(BF16)
            ahead[:, at] = part[1]

        @pl.when(jnp.logical_not(low))
        def _():
            right[:, at] = part[1].astype(BF16)
            left[:, at] = part[2].astype(BF16)
            behind[:, at] = part[3]


def early_kernel(place, hidden, *refs):
    blocks, (packed, total) = refs[:12], refs[12:]
    pack(place, blocks, packed)
    total[...] = jnp.dot(hidden[:, :768], packed[...], preferred_element_type=F32)


def first_kernel(place, hidden, early, *refs):
    blocks, packed, outs = refs[:4], refs[4], refs[5:]
    pack(place, blocks, packed)
    write_sums(early[...] + jnp.dot(hidden[:, 768:], packed[...], preferred_element_type=F32), *outs)


def second_kernel(hidden, early, far, *outs):
    packed = jnp.concatenate([early[...], far[...]], axis=0)
    write_sums(jnp.dot(hidden[...], packed, preferred_element_type=F32), *outs)


def sum_specs(half):
    wide, narrow = (half, NZ * 128), (half, NZ * 64)
    outs = [(wide, BF16), (wide, BF16), (wide, F32), (narrow, F32), (narrow, F32)]
    specs = [pl.BlockSpec((half, 256), lambda i, *_: (0, i))] * 3
    specs.append(pl.BlockSpec((half, 256), lambda i, *_: (0, jnp.minimum(i, 1))))
    specs.append(pl.BlockSpec((half, 256), lambda i, *_: (0, jnp.maximum(i - 2, 0))))
    return [jax.ShapeDtypeStruct(*out) for out in outs], specs


def early_sums(hidden, blocks, place):
    half, tokens = hidden.shape[0] // 2, hidden.shape[1]
    width = blocks[0].shape[1]
    step = width * 2 // NZ
    rows = len(blocks) * 64
    return pl.pallas_call(
        early_kernel,
        out_shape=[jax.ShapeDtypeStruct((rows, width), BF16), jax.ShapeDtypeStruct((half, width), F32)],
        grid_spec=pltpu.PrefetchScalarGridSpec(
            num_scalar_prefetch=1,
            grid=(NZ // 2,),
            in_specs=[pl.BlockSpec((half, tokens), lambda i, o: (0, 0))]
            + [pl.BlockSpec((64, step), lambda i, o: (0, i))] * len(blocks),
            out_specs=[pl.BlockSpec((rows, step), lambda i, o: (0, i)), pl.BlockSpec((half, step), lambda i, o: (0, i))],
        ),
        compiler_params=PARAMS,
        cost_estimate=pl.CostEstimate(flops=2 * half * rows * width, bytes_accessed=20 << 20, transcendentals=0),
        name="early_sums",
    )(place, hidden, *blocks)


def first_sums(hidden, early, blocks, place):
    half, tokens = hidden.shape[0] // 2, hidden.shape[1]
    shapes, specs = sum_specs(half)
    width = blocks[0].shape[1]
    step = width * 2 // NZ
    rows = len(blocks) * 64
    return pl.pallas_call(
        first_kernel,
        out_shape=[jax.ShapeDtypeStruct((rows, width), BF16)] + shapes,
        grid_spec=pltpu.PrefetchScalarGridSpec(
            num_scalar_prefetch=1,
            grid=(NZ // 2,),
            in_specs=[pl.BlockSpec((half, tokens), lambda i, o: (0, 0)), pl.BlockSpec((half, step), lambda i, o: (0, i))]
            + [pl.BlockSpec((64, step), lambda i, o: (0, i))] * len(blocks),
            out_specs=[pl.BlockSpec((rows, step), lambda i, o: (0, i))] + specs,
        ),
        compiler_params=PARAMS,
        cost_estimate=pl.CostEstimate(flops=2 * half * rows * width, bytes_accessed=16 << 20, transcendentals=0),
        name="first_sums",
    )(place, hidden, early, *blocks)


def second_sums(hidden, early, far):
    half, tokens = hidden.shape[0] // 2, hidden.shape[1]
    shapes, specs = sum_specs(half)
    width = early.shape[1]
    step = width * 2 // NZ
    return pl.pallas_call(
        second_kernel,
        out_shape=shapes,
        grid=(NZ // 2,),
        in_specs=[
            pl.BlockSpec((half, tokens), lambda i: (1, 0)),
            pl.BlockSpec((early.shape[0], step), lambda i: (0, i)),
            pl.BlockSpec((far.shape[0], step), lambda i: (0, i)),
        ],
        out_specs=specs,
        compiler_params=PARAMS,
        cost_estimate=pl.CostEstimate(flops=2 * half * tokens * width, bytes_accessed=16 << 20, transcendentals=0),
        name="second_sums",
    )(hidden, early, far)


def input_grad_kernel(where, pairs, gate, up, early, far, *refs):
    weights, (gate_out, up_out) = refs[: NZ + 1], refs[NZ + 1 :]
    weights = [(k, 0, weights[k]) for k in (0, 1, 2, 3, 5, 6, 7)] + [(4, 0, weights[4]), (4, 256, weights[NZ])]

    def compute(columns):
        total = None
        for k, first, w in weights:
            at = pl.ds(pl.multiple_of(where[k] * 512 + first, 256), w.shape[0])
            term = jnp.dot(columns[:, at], w[...], preferred_element_type=F32)
            total = term if total is None else total + term
        grad = total * 0.5
        gate_values = gate[...].astype(F32)
        up_values = up[...].astype(F32)
        sig = jax.nn.sigmoid(gate_values)
        up_out[...] = (grad * (gate_values * sig)).astype(BF16)
        gate_out[...] = (grad * up_values * sig * (1.0 + gate_values * (1.0 - sig))).astype(BF16)

    last = pl.program_id(0) == pl.num_programs(0) - 1
    pl.when(jnp.logical_not(last))(lambda: compute(early))
    pl.when(last)(lambda: compute(far))


def input_grads(gate_pre, up_pre, early, far, weights, where, pairs):
    tokens, width = gate_pre.shape
    rows = 256
    steps = tokens // rows
    tile = pl.BlockSpec((rows, width), lambda i, w, p: (p[i], 0))
    return pl.pallas_call(
        input_grad_kernel,
        out_shape=[jax.ShapeDtypeStruct((tokens, width), BF16)] * 2,
        grid_spec=pltpu.PrefetchScalarGridSpec(
            num_scalar_prefetch=2,
            grid=(steps,),
            in_specs=[
                tile,
                tile,
                pl.BlockSpec((rows, early.shape[1]), lambda i, w, p: (jnp.minimum(i, steps - 2), 0)),
                pl.BlockSpec((rows, far.shape[1]), lambda i, w, p: (0, 0)),
            ]
            + [pl.BlockSpec(w.shape, lambda i, w, p: (0, 0)) for w in weights],
            out_specs=[tile, tile],
        ),
        compiler_params=PARAMS,
        cost_estimate=pl.CostEstimate(
            flops=2 * tokens * width * early.shape[1], bytes_accessed=24 << 20, transcendentals=0
        ),
        name="input_grads",
    )(where, pairs, gate_pre, up_pre, early, far, *weights)


def join_kernel(*refs):
    for k, ref in enumerate(refs[:-1]):
        refs[-1][k * 128 : (k + 1) * 128, :] = ref[...]


def join(parts):
    rows, width = parts[0].shape
    return pl.pallas_call(
        join_kernel,
        out_shape=jax.ShapeDtypeStruct((rows * len(parts), width), parts[0].dtype),
        compiler_params=PARAMS,
        name="join",
    )(*parts)


def gather_tokens(top, bottom):
    behind_top = shift(top, "x", 1)
    ahead_bottom = shift(bottom, "x", -1)
    behind_bottom = shift(bottom, "x", 1)
    ahead_top = shift(top, "x", -1)
    far_top = shift(behind_top, "x", 1)
    far_bottom = shift(ahead_bottom, "x", -1)
    blocks = []
    for half in ((top, bottom), (behind_top, behind_bottom), (ahead_top, ahead_bottom), (far_top, far_bottom)):
        blocks.extend(half)
        blocks.extend(swap(h) for h in half)
    return blocks


def gather_weights(weight):
    behind = shift(weight, "y", 1)
    ahead = shift(weight, "y", -1)
    far = shift(weight, "y", 2)
    here = join([weight, ahead, far, behind])
    parts = {0: here}
    up, down = here, here
    for hop in range(1, 4):
        up = shift(up, "z", 1)
        down = shift(down, "z", -1)
        parts[NZ - hop] = up
        parts[hop] = down
    rows = here.shape[0] // 2
    parts[4] = shift(up[:rows], "z", 1)
    parts[NZ] = shift(down[rows:], "z", -1)
    return [parts[k] for k in range(NZ + 1)]


def sum_over_fs(right, left, mine, ahead, behind):
    half = mine.shape[1] // 2
    right = shift(right, "y", 1)
    left = shift(left, "y", -1)
    up = shift((ahead + right[:, :half].astype(F32)).astype(BF16), "y", 1)
    down = shift((behind + left[:, half:].astype(F32)).astype(BF16), "y", -1)
    pieces = pl.pallas_call(
        pieces_kernel,
        out_shape=jax.ShapeDtypeStruct((NZ, mine.shape[0], 128), BF16),
        compiler_params=PARAMS,
        name="pieces",
    )(mine, right, left, up, down)
    pieces = lax.all_to_all(pieces, "z", 0, 0)
    return jnp.sum(pieces.astype(F32), axis=0)


def pieces_kernel(mine, right, left, up, down, out):
    half = mine.shape[1] // 2
    for k in range(NZ):
        at = slice(k * 128, (k + 1) * 128)
        there = slice(k * 128 % half, k * 128 % half + 128)
        one, two = (up[:, there], left[:, at]) if k < 4 else (right[:, at], down[:, there])
        out[k] = (mine[:, at] + one.astype(F32) + two.astype(F32)).astype(BF16)


def step(cotangent, gate_pre, up_pre, down_weight):
    z, y, x, c = (lax.axis_index(a) for a in ("z", "y", "x", "c"))
    token_total = gate_pre.shape[0] * NZ * NY
    grad_scale = 0.5 / math.sqrt(token_total)
    pairs = ((x + jnp.array([0, 3, 1, 2], jnp.int32)) % NX).astype(jnp.int32)
    where = ((z + jnp.arange(NZ, dtype=jnp.int32)) % NZ).astype(jnp.int32)
    place = jnp.stack([c, y]).astype(jnp.int32)

    half = cotangent.shape[0] // 2
    blocks = gather_tokens(cotangent[:half], cotangent[half:])
    weights = gather_weights(down_weight)
    hidden = hidden_transposed(gate_pre, up_pre, pairs)
    early, sums = early_sums(hidden, blocks[:12], place)
    far, *sums = first_sums(hidden, sums, blocks[12:], place)
    first = sum_over_fs(*sums)
    sums = second_sums(hidden, early, far)
    second = sum_over_fs(*sums)
    gate_grad, up_grad = input_grads(gate_pre, up_pre, early, far, weights, where, pairs)
    down_grad = jnp.concatenate([first, second], axis=0).T * grad_scale
    return gate_grad, up_grad, down_grad


def solution(mesh):
    torus = Mesh(mesh.devices.reshape(NZ, NY, NX, NC), ("z", "y", "x", "c"))
    fs, tp = ("z", "y"), ("x", "c")
    return jax.shard_map(
        step,
        mesh=torus,
        in_specs=(P(fs + tp, None), P(fs, tp), P(fs, tp), P(fs, tp)),
        out_specs=(P(fs, tp), P(fs, tp), P(fs, tp)),
        check_vma=False,
    )
```

```python
import math

import jax
import jax.numpy as jnp
from jax import lax
from jax.experimental import pallas as pl
from jax.experimental.pallas import tpu as pltpu
from jax.sharding import Mesh
from jax.sharding import PartitionSpec as P


BF16 = jnp.bfloat16
F32 = jnp.float32
NZ, NY, NX, NC = 8, 4, 4, 2
PARAMS = pltpu.CompilerParams(vmem_limit_bytes=56 * 1024 * 1024)


def shift(value, axis, step):
    size = lax.axis_size(axis)
    return lax.ppermute(value, axis, [(i, (i + step) % size) for i in range(size)])


def swap(value):
    return lax.ppermute(value, "c", [(0, 1), (1, 0)])


def hidden_kernel(gate, up, out):
    gate_values = gate[...].astype(F32)
    hidden = gate_values * jax.nn.sigmoid(gate_values) * up[...].astype(F32)
    out[...] = hidden.T.astype(BF16)


def hidden_transposed(gate_pre, up_pre, pairs):
    tokens, width = gate_pre.shape
    return pl.pallas_call(
        lambda order, gate, up, out: hidden_kernel(gate, up, out),
        out_shape=jax.ShapeDtypeStruct((width, tokens), BF16),
        grid_spec=pltpu.PrefetchScalarGridSpec(
            num_scalar_prefetch=1,
            grid=(tokens // 256,),
            in_specs=[pl.BlockSpec((256, width), lambda i, o: (o[i], 0))] * 2,
            out_specs=pl.BlockSpec((width, 256), lambda i, o: (0, i)),
        ),
        compiler_params=PARAMS,
        name="hidden",
    )(pairs, gate_pre, up_pre)


def token_rows(place, b):
    pair, rest = divmod(b, 4)
    core, half = divmod(rest, 2)
    return pl.ds(pl.multiple_of(pair * 256 + (place[0] + core) % 2 * 128 + half * 64, 64), 64)


def pack(place, blocks, packed):
    for b, block in enumerate(blocks):
        at = token_rows(place, b)
        for j in range(NY):
            lane = (place[1] + j) % NY * 128
            for q in range(2):
                here = pl.ds(pl.multiple_of(q * 512 + lane, 128), 128)
                packed[at, q * 512 + j * 128 : q * 512 + (j + 1) * 128] = block[:, here]


def write_sums(product, right, left, mine, ahead, behind):
    low = pl.program_id(0) < NZ // 4
    for q in range(2):
        part = [product[:, q * 512 + j * 128 : q * 512 + (j + 1) * 128] for j in range(NY)]
        at = slice(q * 128, (q + 1) * 128)
        mine[:, at] = part[0]

        @pl.when(low)
        def _():
            right[:, at] = part[2].astype(BF16)
            left[:, at] = part[3].astype(BF16)
            ahead[:, at] = part[1]

        @pl.when(jnp.logical_not(low))
        def _():
            right[:, at] = part[1].astype(BF16)
            left[:, at] = part[2].astype(BF16)
            behind[:, at] = part[3]


def send_kernel(place, hidden, *refs):
    blocks, (right, left), columns = refs[:16], refs[16:18], refs[18]
    nearest = jnp.where(pl.program_id(0) < NZ // 4, 2, 1)
    for b, block in enumerate(blocks):
        at = token_rows(place, b)
        for q in range(2):
            for t in range(2):
                lane = q * 512 + (place[1] + nearest + t) % NY * 128
                here = slice(q * 256 + t * 128, q * 256 + (t + 1) * 128)
                columns[at, here] = block[:, pl.ds(pl.multiple_of(lane, 128), 128)]
    product = jnp.dot(hidden[...], columns[...], preferred_element_type=F32)
    for q in range(2):
        at = slice(q * 128, (q + 1) * 128)
        right[:, at] = product[:, q * 256 : q * 256 + 128].astype(BF16)
        left[:, at] = product[:, q * 256 + 128 : q * 256 + 256].astype(BF16)


def rest_kernel(place, hidden, *refs):
    blocks, packed, (mine, ahead, behind), outs = refs[:16], refs[16], refs[17:20], refs[20:]
    half = hidden.shape[0] // 2
    pack(place, blocks, packed)
    write_sums(jnp.dot(hidden[half:, :], packed[...], preferred_element_type=F32), *outs)
    low = pl.program_id(0) < NZ // 4

    def compute(other, out):
        for q in range(2):
            first, second = q * 512, q * 512 + other * 128
            columns = jnp.concatenate([packed[:, first : first + 128], packed[:, second : second + 128]], axis=1)
            product = jnp.dot(hidden[:half, :], columns, preferred_element_type=F32)
            mine[:, q * 128 : (q + 1) * 128] = product[:, :128]
            out[:, q * 128 : (q + 1) * 128] = product[:, 128:]

    pl.when(low)(lambda: compute(1, ahead))
    pl.when(jnp.logical_not(low))(lambda: compute(3, behind))


def sum_specs(half):
    wide, narrow = (half, NZ * 128), (half, NZ * 64)
    outs = [(wide, BF16), (wide, BF16), (wide, F32), (narrow, F32), (narrow, F32)]
    specs = [pl.BlockSpec((half, 256), lambda i, *_: (0, i))] * 3
    specs.append(pl.BlockSpec((half, 256), lambda i, *_: (0, jnp.minimum(i, 1))))
    specs.append(pl.BlockSpec((half, 256), lambda i, *_: (0, jnp.maximum(i - 2, 0))))
    return [jax.ShapeDtypeStruct(*out) for out in outs], specs


def send_sums(hidden, blocks, place):
    half, tokens = hidden.shape[0] // 2, hidden.shape[1]
    shapes, specs = sum_specs(half)
    width = blocks[0].shape[1]
    step = width * 2 // NZ
    return pl.pallas_call(
        send_kernel,
        out_shape=shapes[:2],
        grid_spec=pltpu.PrefetchScalarGridSpec(
            num_scalar_prefetch=1,
            grid=(NZ // 2,),
            in_specs=[pl.BlockSpec((half, tokens), lambda i, o: (0, 0))]
            + [pl.BlockSpec((64, step), lambda i, o: (0, i))] * len(blocks),
            out_specs=specs[:2],
            scratch_shapes=[pltpu.VMEM((tokens, step // 2), BF16)],
        ),
        compiler_params=PARAMS,
        cost_estimate=pl.CostEstimate(flops=half * tokens * width, bytes_accessed=12 << 20, transcendentals=0),
        name="send_sums",
    )(place, hidden, *blocks)


def rest_sums(hidden, blocks, place):
    half, tokens = hidden.shape[0] // 2, hidden.shape[1]
    shapes, specs = sum_specs(half)
    width = blocks[0].shape[1]
    step = width * 2 // NZ
    return pl.pallas_call(
        rest_kernel,
        out_shape=[jax.ShapeDtypeStruct((tokens, width), BF16)] + shapes[2:] + shapes,
        grid_spec=pltpu.PrefetchScalarGridSpec(
            num_scalar_prefetch=1,
            grid=(NZ // 2,),
            in_specs=[pl.BlockSpec((2 * half, tokens), lambda i, o: (0, 0))]
            + [pl.BlockSpec((64, step), lambda i, o: (0, i))] * len(blocks),
            out_specs=[pl.BlockSpec((tokens, step), lambda i, o: (0, i))] + specs[2:] + specs,
        ),
        compiler_params=PARAMS,
        cost_estimate=pl.CostEstimate(flops=3 * half * tokens * width, bytes_accessed=26 << 20, transcendentals=0),
        name="rest_sums",
    )(place, hidden, *blocks)


def input_grad_kernel(where, pairs, gate, up, columns, *refs):
    weights, (gate_out, up_out) = refs[: NZ + 1], refs[NZ + 1 :]
    weights = [(k, 0, weights[k]) for k in (0, 1, 2, 3, 5, 6, 7)] + [(4, 0, weights[4]), (4, 256, weights[NZ])]
    total = None
    for k, first, w in weights:
        at = pl.ds(pl.multiple_of(where[k] * 512 + first, 256), w.shape[0])
        term = jnp.dot(columns[:, at], w[...], preferred_element_type=F32)
        total = term if total is None else total + term
    grad = total * 0.5
    gate_values = gate[...].astype(F32)
    up_values = up[...].astype(F32)
    sig = jax.nn.sigmoid(gate_values)
    up_out[...] = (grad * (gate_values * sig)).astype(BF16)
    gate_out[...] = (grad * up_values * sig * (1.0 + gate_values * (1.0 - sig))).astype(BF16)


def input_grads(gate_pre, up_pre, packed, weights, where, pairs):
    tokens, width = gate_pre.shape
    rows = 256
    tile = pl.BlockSpec((rows, width), lambda i, w, p: (p[i], 0))
    return pl.pallas_call(
        input_grad_kernel,
        out_shape=[jax.ShapeDtypeStruct((tokens, width), BF16)] * 2,
        grid_spec=pltpu.PrefetchScalarGridSpec(
            num_scalar_prefetch=2,
            grid=(tokens // rows,),
            in_specs=[tile, tile, pl.BlockSpec((rows, packed.shape[1]), lambda i, w, p: (i, 0))]
            + [pl.BlockSpec(w.shape, lambda i, w, p: (0, 0)) for w in weights],
            out_specs=[tile, tile],
        ),
        compiler_params=PARAMS,
        cost_estimate=pl.CostEstimate(
            flops=2 * tokens * width * packed.shape[1], bytes_accessed=24 << 20, transcendentals=0
        ),
        name="input_grads",
    )(where, pairs, gate_pre, up_pre, packed, *weights)


def join_kernel(*refs):
    for k, ref in enumerate(refs[:-1]):
        refs[-1][k * 128 : (k + 1) * 128, :] = ref[...]


def join(parts):
    rows, width = parts[0].shape
    return pl.pallas_call(
        join_kernel,
        out_shape=jax.ShapeDtypeStruct((rows * len(parts), width), parts[0].dtype),
        compiler_params=PARAMS,
        name="join",
    )(*parts)


def gather_tokens(top, bottom):
    behind_top = shift(top, "x", 1)
    ahead_bottom = shift(bottom, "x", -1)
    behind_bottom = shift(bottom, "x", 1)
    ahead_top = shift(top, "x", -1)
    far_top = shift(behind_top, "x", 1)
    far_bottom = shift(ahead_bottom, "x", -1)
    blocks = []
    for half in ((top, bottom), (behind_top, behind_bottom), (ahead_top, ahead_bottom), (far_top, far_bottom)):
        blocks.extend(half)
        blocks.extend(swap(h) for h in half)
    return blocks


def gather_weights(weight):
    behind = shift(weight, "y", 1)
    ahead = shift(weight, "y", -1)
    far = shift(weight, "y", 2)
    here = join([weight, ahead, far, behind])
    parts = {0: here}
    up, down = here, here
    for hop in range(1, 4):
        up = shift(up, "z", 1)
        down = shift(down, "z", -1)
        parts[NZ - hop] = up
        parts[hop] = down
    rows = here.shape[0] // 2
    parts[4] = shift(up[:rows], "z", 1)
    parts[NZ] = shift(down[rows:], "z", -1)
    return [parts[k] for k in range(NZ + 1)]


def sum_over_fs(right, left, mine, ahead, behind):
    half = mine.shape[1] // 2
    right = shift(right, "y", 1)
    left = shift(left, "y", -1)
    up = shift((ahead + right[:, :half].astype(F32)).astype(BF16), "y", 1)
    down = shift((behind + left[:, half:].astype(F32)).astype(BF16), "y", -1)
    terms = (mine, right, left, up, down)
    rows = 128
    pieces = pl.pallas_call(
        pieces_kernel,
        out_shape=jax.ShapeDtypeStruct((NZ, mine.shape[0], 128), BF16),
        grid=(mine.shape[0] // rows,),
        in_specs=[pl.BlockSpec((rows, term.shape[1]), lambda i: (i, 0)) for term in terms],
        out_specs=pl.BlockSpec((NZ, rows, 128), lambda i: (0, i, 0)),
        compiler_params=PARAMS,
        name="pieces",
    )(*terms)
    pieces = lax.all_to_all(pieces, "z", 0, 0)
    return jnp.sum(pieces.astype(F32), axis=0)


def pieces_kernel(mine, right, left, up, down, out):
    half = mine.shape[1] // 2
    for k in range(NZ):
        at = slice(k * 128, (k + 1) * 128)
        there = slice(k * 128 % half, k * 128 % half + 128)
        one, two = (up[:, there], left[:, at]) if k < 4 else (right[:, at], down[:, there])
        out[k] = (mine[:, at] + one.astype(F32) + two.astype(F32)).astype(BF16)


def step(cotangent, gate_pre, up_pre, down_weight):
    z, y, x, c = (lax.axis_index(a) for a in ("z", "y", "x", "c"))
    token_total = gate_pre.shape[0] * NZ * NY
    grad_scale = 0.5 / math.sqrt(token_total)
    pairs = ((x + jnp.array([0, 3, 1, 2], jnp.int32)) % NX).astype(jnp.int32)
    where = ((z + jnp.arange(NZ, dtype=jnp.int32)) % NZ).astype(jnp.int32)
    place = jnp.where(jnp.arange(2, dtype=jnp.int32) == 0, c, y).astype(jnp.int32)
    pairs, where, place = lax.optimization_barrier((pairs, where, place))

    half = cotangent.shape[0] // 2
    blocks = gather_tokens(cotangent[:half], cotangent[half:])
    weights = gather_weights(down_weight)
    hidden = hidden_transposed(gate_pre, up_pre, pairs)
    sent = send_sums(hidden, blocks, place)
    packed, *sums = rest_sums(hidden, blocks, place)
    first = sum_over_fs(*sent, *sums[:3])
    second = sum_over_fs(*sums[3:])
    gate_grad, up_grad = input_grads(gate_pre, up_pre, packed, weights, where, pairs)
    down_grad = jnp.concatenate([first, second], axis=0).T * grad_scale
    return gate_grad, up_grad, down_grad


def solution(mesh):
    torus = Mesh(mesh.devices.reshape(NZ, NY, NX, NC), ("z", "y", "x", "c"))
    fs, tp = ("z", "y"), ("x", "c")
    return jax.shard_map(
        step,
        mesh=torus,
        in_specs=(P(fs + tp, None), P(fs, tp), P(fs, tp), P(fs, tp)),
        out_specs=(P(fs, tp), P(fs, tp), P(fs, tp)),
        check_vma=False,
    )
```

```python
import math

import jax
import jax.numpy as jnp
from jax import lax
from jax.experimental import pallas as pl
from jax.experimental.pallas import tpu as pltpu
from jax.sharding import Mesh
from jax.sharding import PartitionSpec as P


BF16 = jnp.bfloat16
F32 = jnp.float32
NZ, NY, NX, NC = 8, 4, 4, 2
PARAMS = pltpu.CompilerParams(vmem_limit_bytes=56 * 1024 * 1024)


def shift(value, axis, step):
    size = lax.axis_size(axis)
    return lax.ppermute(value, axis, [(i, (i + step) % size) for i in range(size)])


def swap(value):
    return lax.ppermute(value, "c", [(0, 1), (1, 0)])


def hidden_kernel(gate, up, out):
    gate_values = gate[...].astype(F32)
    hidden = gate_values * jax.nn.sigmoid(gate_values) * up[...].astype(F32)
    out[...] = hidden.T.astype(BF16)


def hidden_transposed(gate_pre, up_pre, pairs):
    tokens, width = gate_pre.shape
    return pl.pallas_call(
        lambda order, gate, up, out: hidden_kernel(gate, up, out),
        out_shape=jax.ShapeDtypeStruct((width, tokens), BF16),
        grid_spec=pltpu.PrefetchScalarGridSpec(
            num_scalar_prefetch=1,
            grid=(tokens // 256,),
            in_specs=[pl.BlockSpec((256, width), lambda i, o: (o[i], 0))] * 2,
            out_specs=pl.BlockSpec((width, 256), lambda i, o: (0, i)),
        ),
        compiler_params=PARAMS,
        name="hidden",
    )(pairs, gate_pre, up_pre)


def token_rows(place, b):
    pair, rest = divmod(b, 4)
    core, half = divmod(rest, 2)
    return pl.ds(pl.multiple_of(pair * 256 + (place[0] + core) % 2 * 128 + half * 64, 64), 64)


def pack(place, blocks, packed):
    for b, block in enumerate(blocks):
        at = token_rows(place, b)
        for j in range(NY):
            lane = (place[1] + j) % NY * 128
            for q in range(2):
                here = pl.ds(pl.multiple_of(q * 512 + lane, 128), 128)
                packed[at, q * 512 + j * 128 : q * 512 + (j + 1) * 128] = block[:, here]


def write_sums(product, right, left, mine, ahead, behind):
    low = pl.program_id(0) < NZ // 4
    for q in range(2):
        part = [product[:, q * 512 + j * 128 : q * 512 + (j + 1) * 128] for j in range(NY)]
        at = slice(q * 128, (q + 1) * 128)
        mine[:, at] = part[0]

        @pl.when(low)
        def _():
            right[:, at] = part[2].astype(BF16)
            left[:, at] = part[3].astype(BF16)
            ahead[:, at] = part[1]

        @pl.when(jnp.logical_not(low))
        def _():
            right[:, at] = part[1].astype(BF16)
            left[:, at] = part[2].astype(BF16)
            behind[:, at] = part[3]


def send_kernel(place, hidden, *refs):
    blocks, (right, left), columns = refs[:16], refs[16:18], refs[18]
    nearest = jnp.where(pl.program_id(0) < NZ // 4, 2, 1)
    for b, block in enumerate(blocks):
        at = token_rows(place, b)
        for q in range(2):
            for t in range(2):
                lane = q * 512 + (place[1] + nearest + t) % NY * 128
                here = slice(q * 256 + t * 128, q * 256 + (t + 1) * 128)
                columns[at, here] = block[:, pl.ds(pl.multiple_of(lane, 128), 128)]
    product = jnp.dot(hidden[...], columns[...], preferred_element_type=F32)
    for q in range(2):
        at = slice(q * 128, (q + 1) * 128)
        right[:, at] = product[:, q * 256 : q * 256 + 128].astype(BF16)
        left[:, at] = product[:, q * 256 + 128 : q * 256 + 256].astype(BF16)


def rest_kernel(place, hidden, *refs):
    blocks, packed, (mine, ahead, behind), outs = refs[:16], refs[16], refs[17:20], refs[20:]
    half = hidden.shape[0] // 2
    pack(place, blocks, packed)
    write_sums(jnp.dot(hidden[half:, :], packed[...], preferred_element_type=F32), *outs)
    low = pl.program_id(0) < NZ // 4

    def compute(other, out):
        for q in range(2):
            first, second = q * 512, q * 512 + other * 128
            columns = jnp.concatenate([packed[:, first : first + 128], packed[:, second : second + 128]], axis=1)
            product = jnp.dot(hidden[:half, :], columns, preferred_element_type=F32)
            mine[:, q * 128 : (q + 1) * 128] = product[:, :128]
            out[:, q * 128 : (q + 1) * 128] = product[:, 128:]

    pl.when(low)(lambda: compute(1, ahead))
    pl.when(jnp.logical_not(low))(lambda: compute(3, behind))


def sum_specs(half):
    wide, narrow = (half, NZ * 128), (half, NZ * 64)
    outs = [(wide, BF16), (wide, BF16), (wide, F32), (narrow, F32), (narrow, F32)]
    specs = [pl.BlockSpec((half, 256), lambda i, *_: (0, i))] * 3
    specs.append(pl.BlockSpec((half, 256), lambda i, *_: (0, jnp.minimum(i, 1))))
    specs.append(pl.BlockSpec((half, 256), lambda i, *_: (0, jnp.maximum(i - 2, 0))))
    return [jax.ShapeDtypeStruct(*out) for out in outs], specs


def send_sums(hidden, blocks, place):
    half, tokens = hidden.shape[0] // 2, hidden.shape[1]
    shapes, specs = sum_specs(half)
    width = blocks[0].shape[1]
    step = width * 2 // NZ
    return pl.pallas_call(
        send_kernel,
        out_shape=shapes[:2],
        grid_spec=pltpu.PrefetchScalarGridSpec(
            num_scalar_prefetch=1,
            grid=(NZ // 2,),
            in_specs=[pl.BlockSpec((half, tokens), lambda i, o: (0, 0))]
            + [pl.BlockSpec((64, step), lambda i, o: (0, i))] * len(blocks),
            out_specs=specs[:2],
            scratch_shapes=[pltpu.VMEM((tokens, step // 2), BF16)],
        ),
        compiler_params=PARAMS,
        cost_estimate=pl.CostEstimate(flops=half * tokens * width, bytes_accessed=12 << 20, transcendentals=0),
        name="send_sums",
    )(place, hidden, *blocks)


def rest_sums(hidden, blocks, place):
    half, tokens = hidden.shape[0] // 2, hidden.shape[1]
    shapes, specs = sum_specs(half)
    width = blocks[0].shape[1]
    step = width * 2 // NZ
    return pl.pallas_call(
        rest_kernel,
        out_shape=[jax.ShapeDtypeStruct((tokens, width), BF16)] + shapes[2:] + shapes,
        grid_spec=pltpu.PrefetchScalarGridSpec(
            num_scalar_prefetch=1,
            grid=(NZ // 2,),
            in_specs=[pl.BlockSpec((2 * half, tokens), lambda i, o: (0, 0))]
            + [pl.BlockSpec((64, step), lambda i, o: (0, i))] * len(blocks),
            out_specs=[pl.BlockSpec((tokens, step), lambda i, o: (0, i))] + specs[2:] + specs,
        ),
        compiler_params=PARAMS,
        cost_estimate=pl.CostEstimate(flops=3 * half * tokens * width, bytes_accessed=26 << 20, transcendentals=0),
        name="rest_sums",
    )(place, hidden, *blocks)


def input_grad_kernel(where, pairs, gate, up, columns, *refs):
    weights, (gate_out, up_out) = refs[: NZ + 1], refs[NZ + 1 :]
    weights = [(k, 0, weights[k]) for k in (0, 1, 2, 3, 5, 6, 7)] + [(4, 0, weights[4]), (4, 256, weights[NZ])]
    total = None
    for k, first, w in weights:
        at = pl.ds(pl.multiple_of(where[k] * 512 + first, 256), w.shape[0])
        term = jnp.dot(columns[:, at], w[...], preferred_element_type=F32)
        total = term if total is None else total + term
    grad = total * 0.5
    gate_values = gate[...].astype(F32)
    up_values = up[...].astype(F32)
    sig = jax.nn.sigmoid(gate_values)
    up_out[...] = (grad * (gate_values * sig)).astype(BF16)
    gate_out[...] = (grad * up_values * sig * (1.0 + gate_values * (1.0 - sig))).astype(BF16)


def input_grads(gate_pre, up_pre, packed, weights, where, pairs):
    tokens, width = gate_pre.shape
    rows = 256
    tile = pl.BlockSpec((rows, width), lambda i, w, p: (p[i], 0))
    return pl.pallas_call(
        input_grad_kernel,
        out_shape=[jax.ShapeDtypeStruct((tokens, width), BF16)] * 2,
        grid_spec=pltpu.PrefetchScalarGridSpec(
            num_scalar_prefetch=2,
            grid=(tokens // rows,),
            in_specs=[tile, tile, pl.BlockSpec((rows, packed.shape[1]), lambda i, w, p: (i, 0))]
            + [pl.BlockSpec(w.shape, lambda i, w, p: (0, 0)) for w in weights],
            out_specs=[tile, tile],
        ),
        compiler_params=PARAMS,
        cost_estimate=pl.CostEstimate(
            flops=2 * tokens * width * packed.shape[1], bytes_accessed=24 << 20, transcendentals=0
        ),
        name="input_grads",
    )(where, pairs, gate_pre, up_pre, packed, *weights)


def join_kernel(*refs):
    for k, ref in enumerate(refs[:-1]):
        refs[-1][k * 128 : (k + 1) * 128, :] = ref[...]


def join(parts):
    rows, width = parts[0].shape
    return pl.pallas_call(
        join_kernel,
        out_shape=jax.ShapeDtypeStruct((rows * len(parts), width), parts[0].dtype),
        compiler_params=PARAMS,
        name="join",
    )(*parts)


def gather_tokens(top, bottom):
    behind_top = shift(top, "x", 1)
    ahead_bottom = shift(bottom, "x", -1)
    behind_bottom = shift(bottom, "x", 1)
    ahead_top = shift(top, "x", -1)
    far_top = shift(behind_top, "x", 1)
    far_bottom = shift(ahead_bottom, "x", -1)
    blocks = []
    for half in ((top, bottom), (behind_top, behind_bottom), (ahead_top, ahead_bottom), (far_top, far_bottom)):
        blocks.extend(half)
        blocks.extend(swap(h) for h in half)
    return blocks


def gather_weights(weight):
    behind = shift(weight, "y", 1)
    ahead = shift(weight, "y", -1)
    far = shift(weight, "y", 2)
    here = join([weight, ahead, far, behind])
    parts = {0: here}
    up, down = here, here
    for hop in range(1, 4):
        up = shift(up, "z", 1)
        down = shift(down, "z", -1)
        parts[NZ - hop] = up
        parts[hop] = down
    rows = here.shape[0] // 2
    parts[4] = shift(up[:rows], "z", 1)
    parts[NZ] = shift(down[rows:], "z", -1)
    return [parts[k] for k in range(NZ + 1)]


def sum_over_fs(right, left, mine, ahead, behind):
    half = mine.shape[1] // 2
    right = shift(right, "y", 1)
    left = shift(left, "y", -1)
    up = shift((ahead + right[:, :half].astype(F32)).astype(BF16), "y", 1)
    down = shift((behind + left[:, half:].astype(F32)).astype(BF16), "y", -1)
    pieces = pl.pallas_call(
        pieces_kernel,
        out_shape=jax.ShapeDtypeStruct((NZ, mine.shape[0], 128), BF16),
        compiler_params=PARAMS,
        name="pieces",
    )(mine, right, left, up, down)
    pieces = lax.all_to_all(pieces, "z", 0, 0)
    return jnp.sum(pieces.astype(F32), axis=0)


def pieces_kernel(mine, right, left, up, down, out):
    half = mine.shape[1] // 2
    for k in range(NZ):
        at = slice(k * 128, (k + 1) * 128)
        there = slice(k * 128 % half, k * 128 % half + 128)
        one, two = (up[:, there], left[:, at]) if k < 4 else (right[:, at], down[:, there])
        out[k] = (mine[:, at] + one.astype(F32) + two.astype(F32)).astype(BF16)


def step(cotangent, gate_pre, up_pre, down_weight):
    z, y, x, c = (lax.axis_index(a) for a in ("z", "y", "x", "c"))
    token_total = gate_pre.shape[0] * NZ * NY
    grad_scale = 0.5 / math.sqrt(token_total)
    pairs = ((x + jnp.array([0, 3, 1, 2], jnp.int32)) % NX).astype(jnp.int32)
    where = ((z + jnp.arange(NZ, dtype=jnp.int32)) % NZ).astype(jnp.int32)
    place = jnp.stack([c, y]).astype(jnp.int32)

    half = cotangent.shape[0] // 2
    blocks = gather_tokens(cotangent[:half], cotangent[half:])
    weights = gather_weights(down_weight)
    hidden = hidden_transposed(gate_pre, up_pre, pairs)
    sent = send_sums(hidden, blocks, place)
    packed, *sums = rest_sums(hidden, blocks, place)
    first = sum_over_fs(*sent, *sums[:3])
    second = sum_over_fs(*sums[3:])
    gate_grad, up_grad = input_grads(gate_pre, up_pre, packed, weights, where, pairs)
    down_grad = jnp.concatenate([first, second], axis=0).T * grad_scale
    return gate_grad, up_grad, down_grad


def solution(mesh):
    torus = Mesh(mesh.devices.reshape(NZ, NY, NX, NC), ("z", "y", "x", "c"))
    fs, tp = ("z", "y"), ("x", "c")
    return jax.shard_map(
        step,
        mesh=torus,
        in_specs=(P(fs + tp, None), P(fs, tp), P(fs, tp), P(fs, tp)),
        out_specs=(P(fs, tp), P(fs, tp), P(fs, tp)),
        check_vma=False,
    )
```
